32 devices in a mesh: sp: 8 (over z, y), tp: 4 (over x, core).
Axes of the slice: x: 2, y: 2, z: 4, core: 2. Of those that a mesh axis runs over, the one named last changes fastest.
Arguments:
- mixer_output_stream: bfloat16 [1024, 2048], P('sp', 'tp'), may hold values from -6 to 6
- layer_output_gradient: bfloat16 [1024, 2048], P('sp', 'tp'), may hold values from -2.5 to 2.5
- routes: int32 [1024, 2], P('sp'), may hold values from 0 to 7, all different within a row; in each aligned block of 128 rows (0 to 127, 128 to 255, ...) at most 48 rows name the same one
- expert_combine_weight: float32 [1024, 2], P('sp'), may hold values from 0.2 to 1
- expert_gate_weight: bfloat16 [8, 2048, 3584], P('sp', None, 'tp'), may hold values from -0.125 to 0.125
- expert_up_weight: bfloat16 [8, 2048, 3584], P('sp', None, 'tp'), may hold values from -0.125 to 0.125
- expert_down_weight: bfloat16 [8, 3584, 2048], P('sp', 'tp'), may hold values from -0.09375 to 0.09375
- head_mixer_input: bfloat16 [1024, 4096], P('sp', 'tp'), may hold values from -6 to 6
- head_step_size: float32 [1024, 64], P('sp', 'tp'), may hold values from 0.25 to 4
- head_decay_rate: float32 [64], P('tp'), may hold values from 0 to 1
- extra_log_decay: float32 [1024, 64], P('sp', 'tp'), may hold values from -3 to 0
- state_entering_span: float32 [64, 64, 128], P('tp'), may hold values from -48 to 48
- state_input_vectors: bfloat16 [1024, 1024], P('sp', 'tp'), may hold values from -1.75 to 1.75
- state_readout_vectors: bfloat16 [1024, 1024], P('sp', 'tp'), may hold values from -1.75 to 1.75
- gate_preactivation: bfloat16 [1024, 4096], P('sp', 'tp'), may hold values from -6 to 6
- group_norm_scale: float32 [4096], P('tp'), may hold values from 0.1 to 1.9
- mixer_output_weight: bfloat16 [4096, 2048], P('tp', 'sp'), may hold values from -0.09375 to 0.09375
Outputs:
- grad_gate: bfloat16 [8, 2048, 3584], P('sp', None, 'tp')
- grad_up: bfloat16 [8, 2048, 3584], P('sp', None, 'tp')
- grad_down: bfloat16 [8, 3584, 2048], P('sp', 'tp')
- grad_out_proj: float32 [4096, 2048], P('tp', 'sp')
- grad_input: bfloat16 [1024, 4096], P('sp', 'tp')
- grad_step: float32 [1024, 64], P('sp', 'tp')
- grad_state_in: bfloat16 [1024, 1024], P('sp', 'tp')
- grad_read_out: bfloat16 [1024, 1024], P('sp', 'tp')
- grad_gate_in: bfloat16 [1024, 4096], P('sp', 'tp')
The draws below stay inside these ranges and needn't reach their ends.
Inputs may be any that keep to these rules, and one draw needn't show every extreme that they name: `routes`: the two experts of a token differ. In each aligned block of 128 rows no expert is named more than 48 times, and in every draw some expert is named exactly 48 times in some block.
All inputs are finite; a program needn't handle non-finite values.
Results may differ from the reference program's by a relative error of at most 0.02.
Values may be sent and summed in bfloat16 or wider, within the bound.
No kernel may reach another device: no remote copies, remote signals or barrier semaphores. Data moves between devices by JAX's collectives and lax.ppermute only.
A program may use at most 128 MiB of HBM per device.

```python
import math
from functools import partial
import jax
import jax.numpy as jnp
import numpy as np
from jax import lax

D = 2048
FF = 3584
HEADS = 64
HDIM = 64
GROUPS = 8
STATE = 128
BLK = 128
TOP = 2
TOK_DEV = 128
DI = 4096
EXPERTS = 8
CAP = 48
TOKENS = 1024
N_TP = 4


def draw_head_step_size(key, part):
    first, second = jax.random.split(key)
    rough = jnp.exp(jax.random.uniform(first, (TOKENS, HEADS), jnp.float32, math.log(0.5), math.log(2.0)))
    spans = TOKENS // TOK_DEV
    factor = jnp.exp(jax.random.uniform(second, (spans, 1, 1), jnp.float32, math.log(0.5), math.log(2.0)))
    return (rough.reshape(spans, TOK_DEV, HEADS) * factor).reshape(TOKENS, HEADS)


def draw_head_decay_rate(key, part):
    first, second = jax.random.split(key)
    picks = jax.random.randint(first, (HEADS,), 0, 8)
    limit = 4
    spread = jnp.exp(jax.random.uniform(second, (HEADS,), jnp.float32, math.log(0.5), math.log(2.0)))
    fast_rate = 3.0 / BLK * spread
    slow_rate = 0.25 / TOKENS * spread
    return jnp.where(picks < limit, fast_rate, slow_rate)


def draw_extra_log_decay(key, part):
    first, second = jax.random.split(key)
    places = jax.random.randint(first, (3,), 0, TOKENS)
    amounts = jnp.log(jax.random.uniform(second, (3, HEADS), jnp.float32, 0.5, 0.8))
    hits = (jnp.arange(TOKENS, dtype=jnp.int32)[:, None] == places[None, :]).astype(jnp.float32)
    return jnp.dot(hits, amounts, precision=lax.Precision.HIGHEST)


def strengthened(result, rng, source, target, parts, factor):
    owner, partner = [(jnp.arange(result.shape[dim]) // (result.shape[dim] // parts)).reshape([-1 if axis == dim else 1 for axis in range(result.ndim)]) for dim in (source, target)]
    chosen = jax.random.permutation(rng, parts)[partner]
    strong = (owner == chosen) | (owner == (partner + parts // 2) % parts)
    return jnp.where(strong, factor * result, result)


def level_of(own_key, shape, cuts, smallest, high):
    factor_of, own = 1.0, jax.random.fold_in(own_key, 6)
    for dim, parts in cuts:
        steps = jnp.exp(jax.random.uniform(jax.random.fold_in(own, dim), (parts,), jnp.float32, smallest / len(cuts), high / len(cuts)))
        factor_of = factor_of * jnp.repeat(steps, shape[dim] // parts).reshape([-1 if axis == dim else 1 for axis in range(len(shape))])
    return factor_of


def deal_out(stream_key, own, number, rows, number_of, top, most, slope):
    ranking = jax.random.permutation(stream_key, number_of)
    heavy_load, common = portions_of(number_of, rows * top, most, slope, True), portions_of(number_of, rows * top, most, slope, False)
    places = jnp.arange(number_of)

    def named(sizes, turn):
        used = int((sizes > 0).sum())
        fixed = max(1, used // 4)
        moved = fixed + (places - fixed + turn * (used - fixed)) % max(1, number_of - fixed)
        return jnp.zeros((number_of,), jnp.int32).at[ranking[jnp.where(places < fixed, places, moved)]].set(jnp.asarray(sizes, jnp.int32))

    sizes = jnp.where(number % 4 == 0, named(heavy_load, number // 4), named(common, number - number // 4 - 1))
    mixed = jax.random.permutation(jax.random.fold_in(own, 3), number_of)
    source_of, receiver = mixed[0:number_of // 2 * 2:2], mixed[1:number_of // 2 * 2:2]
    room = jnp.minimum(sizes[source_of] - 1, most - sizes[receiver]) // 2
    room = jnp.where((source_of == ranking[0]) | (receiver == ranking[0]) | (sizes[receiver] == 0), 0, jnp.maximum(room, 0))
    moved = jax.random.randint(jax.random.fold_in(own, 4), (number_of // 2,), 0, 1 << 20) % (room + 1)
    sizes = sizes.at[source_of].add(-moved).at[receiver].add(moved)
    members = jnp.searchsorted(jnp.cumsum(sizes), jnp.arange(rows * top), side="right").astype(jnp.int32)
    table = members.reshape(top, rows).T
    table = table[jax.random.permutation(jax.random.fold_in(own, 1), rows)]
    turn = jax.random.randint(jax.random.fold_in(own, 2), (rows, 1), 0, top)
    return jnp.take_along_axis(table, (jnp.arange(top)[None, :] + turn) % top, axis=1)


def portions_of(number_of, total, bound, slope, full):
    portions = [(1 << 20) // math.isqrt(rank ** slope) + 1 for rank in range(1, number_of + 1)]
    largest = bound if full else min(bound, max(-(-total // number_of), total * portions[0] // sum(portions)))
    least = 1 if total - largest >= number_of - 1 else 0
    counts, spare = [largest] + [least] * (number_of - 1), total - largest - least * (number_of - 1)
    while spare > 0:
        free = [i for i in range(1, number_of) if counts[i] < largest] or [i for i in range(1, number_of) if counts[i] < bound]
        mass, remaining = sum([portions[i] for i in free]), spare
        for i in free:
            addition = min(bound - counts[i], max(1, remaining * portions[i] // mass), spare)
            counts[i] = counts[i] + addition
            spare = spare - addition
    return np.array(counts)


def scatter_about(stream_key, extent, deviation, most, pieces=(), held_as=jnp.bfloat16):
    values = deviation * jax.random.normal(stream_key, extent, jnp.float32)
    if pieces:
        values = values * level_of(stream_key, extent, pieces, -0.22, 0.18)
    return jnp.clip(values, -most, most).astype(held_as)


def gaussian_with(key, shape, width, bound, shards, heavy, held_as=jnp.bfloat16):
    entries = width * jax.random.normal(key, shape, jnp.float32)
    if shards:
        entries = entries * level_of(key, shape, shards, -0.22, 0.18)
    return jnp.clip(strengthened(entries, jax.random.fold_in(key, 3), *heavy), -bound, bound).astype(held_as)


def setup_inputs(seed: int = 0) -> dict:
    seeds = jax.random.split(jax.random.key(seed), 18)
    mixer_output_stream = scatter_about(seeds[0], (TOKENS, D), 1.0, 6.0, ((0, 8), (1, 4)))
    layer_output_gradient = gaussian_with(seeds[1], (TOKENS, D), 0.3, 2.5, ((0, 8), (1, 4)), (0, 1, 8, 2.0))
    routes_keys = jax.random.split(jax.random.fold_in(seeds[2], 1), TOKENS // TOK_DEV)
    routes_turns = jax.random.permutation(jax.random.fold_in(seeds[2], 3), TOKENS // TOK_DEV)
    routes = jax.vmap(lambda own, number: deal_out(jax.random.fold_in(seeds[2], 2), own, number, TOK_DEV, EXPERTS, TOP, CAP, 1))(routes_keys, routes_turns).reshape((TOKENS, TOP))
    expert_combine_weight = jnp.clip(0.2 + 0.8 * jax.random.uniform(seeds[3], (TOKENS, TOP), jnp.float32) ** level_of(seeds[3], (TOKENS, TOP), ((0, 8),), -0.2, 0.2), 0.2, 1.0)
    expert_gate_weight = scatter_about(seeds[4], (EXPERTS, D, FF), D ** -0.5, 0.125, ((0, 8), (2, 4)))
    expert_up_weight = scatter_about(seeds[5], (EXPERTS, D, FF), D ** -0.5, 0.125, ((0, 8), (2, 4)))
    expert_down_weight = scatter_about(seeds[6], (EXPERTS, FF, D), FF ** -0.5, 0.09375, ((0, 8), (1, 4)))
    head_mixer_input = scatter_about(seeds[7], (TOKENS, DI), 1.0, 6.0, ((0, 8), (1, 4)))
    head_step_size = draw_head_step_size(jax.random.fold_in(seeds[17], 71), 0)
    head_decay_rate = draw_head_decay_rate(jax.random.fold_in(seeds[17], 71), 0)
    extra_log_decay = draw_extra_log_decay(jax.random.fold_in(seeds[17], 71), 0)
    state_entering_span = scatter_about(seeds[11], (HEADS, HDIM, STATE), 8.0, 48.0, ((0, 4),), jnp.float32)
    state_input_vectors = scatter_about(seeds[12], (TOKENS, GROUPS * STATE), (STATE ** -0.25), 1.75, ((0, 8), (1, 4)))
    state_readout_vectors = scatter_about(seeds[13], (TOKENS, GROUPS * STATE), (STATE ** -0.25), 1.75, ((0, 8), (1, 4)))
    gate_preactivation = scatter_about(seeds[14], (TOKENS, DI), 1.0, 6.0, ((0, 8), (1, 4)))
    group_norm_scale = jnp.clip(1.0 + 0.18 * jax.random.normal(seeds[15], (DI,), jnp.float32), 0.1, 1.9)
    mixer_output_weight = scatter_about(seeds[16], (DI, D), DI ** -0.5, 0.09375, ((0, 4), (1, 8)))
    return dict(mixer_output_stream=mixer_output_stream, layer_output_gradient=layer_output_gradient, routes=routes, expert_combine_weight=expert_combine_weight, expert_gate_weight=expert_gate_weight, expert_up_weight=expert_up_weight, expert_down_weight=expert_down_weight, head_mixer_input=head_mixer_input, head_step_size=head_step_size, head_decay_rate=head_decay_rate, extra_log_decay=extra_log_decay, state_entering_span=state_entering_span, state_input_vectors=state_input_vectors, state_readout_vectors=state_readout_vectors, gate_preactivation=gate_preactivation, group_norm_scale=group_norm_scale, mixer_output_weight=mixer_output_weight)


norm_eps = 1e-05
exact_mode = lax.Precision.HIGHEST

def span_local_scan(input_heads, time_step, decay_speed, sudden_decay, input_vector_groups, readout_groups, starting_state):
    length, head_count, head_size = input_heads.shape
    groups, state_size = (input_vector_groups.shape[1], input_vector_groups.shape[2])
    per_group = head_count // groups
    block_count = length // BLK
    log_decay_total = sudden_decay - time_step * decay_speed[None, :]
    scaled = (input_heads * time_step[:, :, None]).reshape(block_count, BLK, groups, per_group, head_size)
    log_decay_total = log_decay_total.reshape(block_count, BLK, groups, per_group)
    b_rows = input_vector_groups.reshape(block_count, BLK, groups, state_size)
    c_rows = readout_groups.reshape(block_count, BLK, groups, state_size)
    cumulative = jnp.cumsum(log_decay_total, axis=1)
    causal_mask = jnp.tril(jnp.ones((BLK, BLK), dtype=bool))
    cum_t = jnp.moveaxis(cumulative, 1, -1)
    gaps = cum_t[..., :, None] - cum_t[..., None, :]
    decays = jnp.where(causal_mask, jnp.exp(jnp.where(causal_mask, gaps, 0.0)), 0.0)
    affinity = jnp.einsum('blgn,bsgn->bgls', c_rows, b_rows, precision=exact_mode)
    y_diag = jnp.einsum('bghls,bsghp->blghp', affinity[:, :, None] * decays, scaled, precision=exact_mode)
    to_end = jnp.exp(cumulative[:, -1:] - cumulative)
    states = jnp.einsum('blgn,blghp->bghpn', b_rows, scaled * to_end[..., None], precision=exact_mode)
    block_decay = jnp.exp(cumulative[:, -1])

    def advance(running, inputs):
        block_state, decay_now = inputs
        return (decay_now[..., None, None] * running + block_state, running)
    first_state = starting_state.reshape(groups, per_group, head_size, state_size)
    closing_state, incoming_state = lax.scan(advance, first_state, (states, block_decay))
    y_off = jnp.einsum('blgn,bghpn->blghp', c_rows, incoming_state, precision=exact_mode) * jnp.exp(cumulative)[..., None]
    result_rows = (y_diag + y_off).reshape(length, head_count, head_size)
    return (result_rows, closing_state.reshape(head_count, head_size, state_size))

def gate_norm(scan_out, gate_vals, group_norm_scale, groups):
    length = scan_out.shape[0]
    gated = scan_out.reshape(length, -1) * jax.nn.silu(gate_vals)
    grouped = gated.reshape(length, groups, -1)
    factor = lax.rsqrt(lax.optimization_barrier(jnp.mean(grouped * grouped, axis=-1, keepdims=True)) + norm_eps)
    return (grouped * factor).reshape(length, -1) * group_norm_scale[None, :]

def slot_index(route_rows, expert_count, capacity):
    flat_routes = route_rows.reshape(-1)
    onehot = (flat_routes[:, None] == jnp.arange(expert_count, dtype=jnp.int32)[None, :]).astype(jnp.int32)
    before = jnp.cumsum(onehot, axis=0) - onehot
    return flat_routes * capacity + lax.optimization_barrier(jnp.sum(before * onehot, axis=1))

def build_table(destination, slot_count):
    pair_count = destination.shape[0]
    return jnp.full((slot_count,), pair_count, jnp.int32).at[destination].set(jnp.arange(pair_count, dtype=jnp.int32))

def pack_rows(stream, grad_rows, slot_table, weights):
    token_of = slot_table // 2
    routed = jnp.take(stream, token_of, axis=0, mode='fill', fill_value=0)
    weight_of = jnp.take(weights.reshape(-1), slot_table, mode='fill', fill_value=0.0)
    picked = jnp.take(grad_rows, token_of, axis=0, mode='fill', fill_value=0).astype(jnp.float32)
    return (routed, (picked * weight_of[:, None]).astype(jnp.bfloat16))

def expert_hidden(routed_rows, routed_grads, w_gate, w_up, w_down):
    pre_gate = jnp.dot(routed_rows, w_gate, preferred_element_type=jnp.float32)
    pre_up = jnp.dot(routed_rows, w_up, preferred_element_type=jnp.float32)
    activated = jax.nn.silu(pre_gate)
    hidden = (activated * pre_up).astype(jnp.bfloat16)
    hidden_grad = lax.dot_general(routed_grads, w_down, (((1,), (1,)), ((), ())), preferred_element_type=jnp.float32)
    sigmoid_gate = jax.nn.sigmoid(pre_gate)
    gate_grad = (hidden_grad * pre_up * sigmoid_gate * (1.0 + pre_gate * (1.0 - sigmoid_gate))).astype(jnp.bfloat16)
    up_grad = (hidden_grad * activated).astype(jnp.bfloat16)
    return (hidden, gate_grad, up_grad)

def expert_weight_grads(routed_rows, routed_grads, hidden, gate_grad, up_grad):
    contract = (((0,), (0,)), ((), ()))
    grad_g = lax.dot_general(routed_rows, gate_grad, contract, preferred_element_type=jnp.float32)
    grad_u = lax.dot_general(routed_rows, up_grad, contract, preferred_element_type=jnp.float32)
    grad_d = lax.dot_general(hidden, routed_grads, contract, preferred_element_type=jnp.float32)
    return (grad_g.astype(jnp.bfloat16), grad_u.astype(jnp.bfloat16), grad_d.astype(jnp.bfloat16))

def row_partial(gate_grad, up_grad, w_gate, w_up):
    contract = (((1,), (1,)), ((), ()))
    partial_sum = lax.dot_general(gate_grad, w_gate, contract, preferred_element_type=jnp.float32)
    partial_sum = partial_sum + lax.dot_general(up_grad, w_up, contract, preferred_element_type=jnp.float32)
    return lax.optimization_barrier(partial_sum.astype(jnp.bfloat16)).astype(jnp.float32)

def add_returns(grad_rows, returned, destination):
    token_count = grad_rows.shape[0]
    gathered = jnp.take(returned, destination, axis=0).reshape(token_count, -1, returned.shape[-1]).astype(jnp.float32)
    return (grad_rows.astype(jnp.float32) + lax.optimization_barrier(jnp.sum(gathered, axis=1))).astype(jnp.bfloat16)

def reference(mixer_output_stream, layer_output_gradient, routes, expert_combine_weight, expert_gate_weight, expert_up_weight, expert_down_weight, head_mixer_input, head_step_size, head_decay_rate, extra_log_decay, state_entering_span, state_input_vectors, state_readout_vectors, gate_preactivation, group_norm_scale, mixer_output_weight):
    blocks = TOKENS // TOK_DEV
    destination = jax.vmap(partial(slot_index, expert_count=EXPERTS, capacity=CAP))(routes.reshape(blocks, TOK_DEV, TOP))
    tables = jax.vmap(partial(build_table, slot_count=EXPERTS * CAP))(destination)
    sent_rows, sent_grads = jax.vmap(pack_rows)(mixer_output_stream.reshape(blocks, TOK_DEV, D), layer_output_gradient.reshape(blocks, TOK_DEV, D), tables, expert_combine_weight.reshape(blocks, TOK_DEV, TOP))

    def by_expert(values):
        return values.reshape(blocks, EXPERTS, CAP, D).transpose(1, 0, 2, 3).reshape(EXPERTS, blocks * CAP, D)

    def per_expert(packed):
        routed_rows, routed_grads, w_gate, w_up, w_down = packed
        hidden, gate_grad, up_grad = expert_hidden(routed_rows, routed_grads, w_gate, w_up, w_down)
        grad_g, grad_u, grad_d = expert_weight_grads(routed_rows, routed_grads, hidden, gate_grad, up_grad)
        block_width = w_gate.shape[1] // N_TP
        running = jnp.zeros((routed_rows.shape[0], w_gate.shape[0]), jnp.float32)
        for block_number in range(N_TP):
            first_col = block_number * block_width
            running = running + row_partial(gate_grad[:, first_col:first_col + block_width], up_grad[:, first_col:first_col + block_width], w_gate[:, first_col:first_col + block_width], w_up[:, first_col:first_col + block_width])
        return (grad_g, grad_u, grad_d, running.astype(jnp.bfloat16))
    grad_gate, grad_up, grad_down, returned = lax.map(per_expert, (by_expert(sent_rows), by_expert(sent_grads), expert_gate_weight, expert_up_weight, expert_down_weight))
    returned = returned.reshape(EXPERTS, blocks, CAP, D).transpose(1, 0, 2, 3).reshape(blocks, EXPERTS * CAP, D)
    mix_grad = jax.vmap(add_returns)(layer_output_gradient.reshape(blocks, TOK_DEV, D), returned, destination).reshape(TOKENS, D)
    input_heads = head_mixer_input.astype(jnp.float32).reshape(TOKENS, HEADS, HDIM)
    input_vector_groups = state_input_vectors.astype(jnp.float32).reshape(TOKENS, GROUPS, STATE)
    readout_groups = state_readout_vectors.astype(jnp.float32).reshape(TOKENS, GROUPS, STATE)

    def forward(input_values, time_step_values, input_vector_entries, readout_entries):
        result_rows, closing_state = span_local_scan(input_values, time_step_values, head_decay_rate, extra_log_decay, input_vector_entries, readout_entries, state_entering_span)
        return result_rows
    scan_out, pull_back = jax.vjp(forward, input_heads, head_step_size, input_vector_groups, readout_groups)

    def apply_norm(scan_vals, gate_vals):
        return gate_norm(scan_vals, gate_vals, group_norm_scale, GROUPS)
    normed, pull_norm = jax.vjp(apply_norm, scan_out, gate_preactivation.astype(jnp.float32))
    normed_low = normed.astype(jnp.bfloat16)
    grad_out_proj = lax.dot_general(normed_low, mix_grad, (((0,), (0,)), ((), ())), preferred_element_type=jnp.float32)
    normed_grad = lax.dot_general(mix_grad, mixer_output_weight, (((1,), (1,)), ((), ())), preferred_element_type=jnp.float32)
    scanned_gradient, gate_grad_in = pull_norm(normed_grad)
    input_grad, step_grad, b_grad, c_grad = pull_back(scanned_gradient)
    return (grad_gate, grad_up, grad_down, grad_out_proj, input_grad.reshape(TOKENS, DI).astype(jnp.bfloat16), step_grad, b_grad.reshape(TOKENS, GROUPS * STATE).astype(jnp.bfloat16), c_grad.reshape(TOKENS, GROUPS * STATE).astype(jnp.bfloat16), gate_grad_in.astype(jnp.bfloat16))
```

```python
import jax
import jax.numpy as jnp
from jax import lax
from jax.sharding import PartitionSpec as P

HDIM = 64
STATE = 128
BLK = 128


norm_eps = 1e-05
exact_mode = lax.Precision.HIGHEST


def swapped(x, axis, mask):
    n = lax.axis_size(axis)
    return lax.ppermute(x, axis, [(i, i ^ mask) for i in range(n)])


def bits_of(n):
    return [1 << k for k in range(n.bit_length() - 1)]


def reorder(blocks, me, n):
    blocks = list(blocks)
    for bit in bits_of(n):
        is_set = (me & bit) != 0
        for m in range(n):
            if not m & bit:
                a, b = blocks[m], blocks[m | bit]
                blocks[m], blocks[m | bit] = jnp.where(is_set, b, a), jnp.where(is_set, a, b)
    return blocks


def gather_relative(x, axis):
    n = lax.axis_size(axis)
    blocks = {0: x}
    for bit in reversed(bits_of(n)):
        for m in sorted(blocks):
            blocks[m | bit] = swapped(blocks[m], axis, bit)
    return [blocks[m] for m in range(n)]


def exchange_relative(blocks, axis):
    return [blocks[0]] + [swapped(blocks[m], axis, m) for m in range(1, len(blocks))]


def gather_columns(x, axis):
    n = lax.axis_size(axis)
    return jnp.concatenate(reorder(gather_relative(x, axis), lax.axis_index(axis), n), axis=1)


def scatter_sum_columns(x, axis):
    n = lax.axis_size(axis)
    width = x.shape[1] // n
    held = [x[:, j * width : (j + 1) * width] for j in range(n)]
    held = dict(enumerate(reorder(held, lax.axis_index(axis), n)))
    for bit in bits_of(n):
        going = [m for m in held if m & bit]
        sent = jnp.concatenate([held[m].astype(jnp.bfloat16) for m in going], axis=1)
        got = swapped(sent, axis, bit).astype(jnp.float32)
        for at, m in enumerate(going):
            held[m ^ bit] = held[m ^ bit] + got[:, at * width : (at + 1) * width]
            del held[m]
    return held[0].astype(jnp.bfloat16)


def scaled_by(log_scale, state):
    return jnp.exp(log_scale)[:, None, None] * state


def state_before(total, logs, axis):
    n, me = lax.axis_size(axis), lax.axis_index(axis)
    prefix = jnp.zeros_like(total)
    gap = jnp.zeros_like(logs[0])
    for bit in bits_of(n):
        upper = (me & bit) != 0
        mine, other = sum(logs[:bit]), sum(logs[bit : 2 * bit])
        got = swapped(total.astype(jnp.bfloat16), axis, bit).astype(jnp.float32)
        prefix = prefix + jnp.where(upper, scaled_by(gap, got), 0.0)
        gap = gap + jnp.where(upper, other, 0.0)
        if 2 * bit < n:
            total = jnp.where(
                upper, scaled_by(mine, got) + total, scaled_by(other, total) + got
            )
    return prefix, gap


def state_after(total, logs, axis):
    n, me = lax.axis_size(axis), lax.axis_index(axis)
    suffix = jnp.zeros_like(total)
    gap = jnp.zeros_like(logs[0])
    for bit in bits_of(n):
        upper = (me & bit) != 0
        mine, other = sum(logs[:bit]), sum(logs[bit : 2 * bit])
        got = swapped(total.astype(jnp.bfloat16), axis, bit).astype(jnp.float32)
        suffix = suffix + jnp.where(upper, 0.0, scaled_by(gap, got))
        gap = gap + jnp.where(upper, 0.0, other)
        if 2 * bit < n:
            total = jnp.where(
                upper, got + scaled_by(other, total), total + scaled_by(mine, got)
            )
    return suffix


def span_local_scan(
    input_heads,
    time_step,
    decay_speed,
    sudden_decay,
    input_vector_groups,
    readout_groups,
    starting_state,
):
    length, head_count, head_size = input_heads.shape
    groups, state_size = (input_vector_groups.shape[1], input_vector_groups.shape[2])
    per_group = head_count // groups
    block_count = length // BLK
    log_decay_total = sudden_decay - time_step * decay_speed[None, :]
    scaled = (input_heads * time_step[:, :, None]).reshape(
        block_count, BLK, groups, per_group, head_size
    )
    log_decay_total = log_decay_total.reshape(block_count, BLK, groups, per_group)
    b_rows = input_vector_groups.reshape(block_count, BLK, groups, state_size)
    c_rows = readout_groups.reshape(block_count, BLK, groups, state_size)
    cumulative = jnp.cumsum(log_decay_total, axis=1)
    causal_mask = jnp.tril(jnp.ones((BLK, BLK), dtype=bool))
    cum_t = jnp.moveaxis(cumulative, 1, -1)
    gaps = cum_t[..., :, None] - cum_t[..., None, :]
    decays = jnp.where(causal_mask, jnp.exp(jnp.where(causal_mask, gaps, 0.0)), 0.0)
    affinity = jnp.einsum("blgn,bsgn->bgls", c_rows, b_rows, precision=exact_mode)
    y_diag = jnp.einsum(
        "bghls,bsghp->blghp", affinity[:, :, None] * decays, scaled, precision=exact_mode
    )
    to_end = jnp.exp(cumulative[:, -1:] - cumulative)
    states = jnp.einsum(
        "blgn,blghp->bghpn", b_rows, scaled * to_end[..., None], precision=exact_mode
    )
    block_decay = jnp.exp(cumulative[:, -1])

    def advance(running, inputs):
        block_state, decay_now = inputs
        return (decay_now[..., None, None] * running + block_state, running)

    first_state = starting_state.reshape(groups, per_group, head_size, state_size)
    closing_state, incoming_state = lax.scan(advance, first_state, (states, block_decay))
    y_off = (
        jnp.einsum("blgn,bghpn->blghp", c_rows, incoming_state, precision=exact_mode)
        * jnp.exp(cumulative)[..., None]
    )
    result_rows = (y_diag + y_off).reshape(length, head_count, head_size)
    return (result_rows, closing_state.reshape(head_count, head_size, state_size))


def span_final_state(input_heads, time_step, decay_speed, sudden_decay, input_vector_groups):
    length, head_count, head_size = input_heads.shape
    groups = input_vector_groups.shape[1]
    log_decay_total = sudden_decay - time_step * decay_speed[None, :]
    sum_total = jnp.sum(log_decay_total, axis=0)
    after = sum_total[None, :] - jnp.cumsum(log_decay_total, axis=0)
    weighted = (input_heads * (time_step * jnp.exp(after))[:, :, None]).reshape(
        length, groups, head_count // groups, head_size
    )
    result = jnp.einsum("tgn,tghp->ghpn", input_vector_groups, weighted, precision=exact_mode)
    return (result.reshape(head_count, head_size, -1), sum_total)


def carried_weight(scanned_gradient, readout_groups, time_step, decay_speed, sudden_decay):
    length, head_count, head_size = scanned_gradient.shape
    groups = readout_groups.shape[1]
    log_decay_total = sudden_decay - time_step * decay_speed[None, :]
    weighted = (
        scanned_gradient * jnp.exp(jnp.cumsum(log_decay_total, axis=0))[:, :, None]
    ).reshape(length, groups, head_count // groups, head_size)
    result = jnp.einsum("tgn,tghp->ghpn", readout_groups, weighted, precision=exact_mode)
    return result.reshape(head_count, head_size, -1)


def gate_norm(scan_out, gate_vals, group_norm_scale, groups):
    length = scan_out.shape[0]
    gated = scan_out.reshape(length, -1) * jax.nn.silu(gate_vals)
    grouped = gated.reshape(length, groups, -1)
    factor = lax.rsqrt(jnp.mean(grouped * grouped, axis=-1, keepdims=True) + norm_eps)
    return (grouped * factor).reshape(length, -1) * group_norm_scale[None, :]


def pair_slots(relative, weights, expert_count, capacity):
    token_count = relative.shape[0]
    chosen = relative[:, :, None] == jnp.arange(expert_count, dtype=jnp.int32)[None, None, :]
    mask = jnp.any(chosen, axis=1)
    weight_of = jnp.sum(jnp.where(chosen, weights[:, :, None], 0.0), axis=1)
    earlier = jnp.tril(jnp.ones((token_count, token_count), jnp.bfloat16), -1)
    place = jnp.dot(earlier, mask.astype(jnp.bfloat16), preferred_element_type=jnp.float32)
    place = jnp.where(mask, place.astype(jnp.int32), -1).T
    at_slot = place[:, None, :] == jnp.arange(capacity, dtype=jnp.int32)[None, :, None]
    slot_weight = jnp.sum(jnp.where(at_slot, weight_of.T[:, None, :], 0.0), axis=2)
    select = at_slot.astype(jnp.bfloat16).reshape(expert_count * capacity, token_count)
    return select, slot_weight.reshape(-1, 1)


def pack_rows(stream, grad_rows, select, slot_weight):
    routed = jnp.dot(select, stream, preferred_element_type=jnp.float32).astype(jnp.bfloat16)
    picked = jnp.dot(select, grad_rows, preferred_element_type=jnp.float32)
    return jnp.concatenate([routed, (picked * slot_weight).astype(jnp.bfloat16)], axis=1)


def expert_hidden(routed_rows, routed_grads, w_gate, w_up, w_down):
    pre_gate = jnp.dot(routed_rows, w_gate, preferred_element_type=jnp.float32)
    pre_up = jnp.dot(routed_rows, w_up, preferred_element_type=jnp.float32)
    activated = jax.nn.silu(pre_gate)
    hidden = (activated * pre_up).astype(jnp.bfloat16)
    hidden_grad = lax.dot_general(
        routed_grads, w_down, (((1,), (1,)), ((), ())), preferred_element_type=jnp.float32
    )
    sigmoid_gate = jax.nn.sigmoid(pre_gate)
    gate_grad = (
        hidden_grad * pre_up * sigmoid_gate * (1.0 + pre_gate * (1.0 - sigmoid_gate))
    ).astype(jnp.bfloat16)
    up_grad = (hidden_grad * activated).astype(jnp.bfloat16)
    return (hidden, gate_grad, up_grad)


def expert_weight_grads(routed_rows, routed_grads, hidden, gate_grad, up_grad):
    contract = (((0,), (0,)), ((), ()))
    grad_g = lax.dot_general(routed_rows, gate_grad, contract, preferred_element_type=jnp.float32)
    grad_u = lax.dot_general(routed_rows, up_grad, contract, preferred_element_type=jnp.float32)
    grad_d = lax.dot_general(hidden, routed_grads, contract, preferred_element_type=jnp.float32)
    return (grad_g.astype(jnp.bfloat16), grad_u.astype(jnp.bfloat16), grad_d.astype(jnp.bfloat16))


def row_partial(gate_grad, up_grad, w_gate, w_up):
    contract = (((1,), (1,)), ((), ()))
    partial_sum = lax.dot_general(gate_grad, w_gate, contract, preferred_element_type=jnp.float32)
    return partial_sum + lax.dot_general(
        up_grad, w_up, contract, preferred_element_type=jnp.float32
    )


def add_returns(grad_rows, returned, select):
    added = lax.dot_general(
        select, returned, (((0,), (0,)), ((), ())), preferred_element_type=jnp.float32
    )
    return (grad_rows.astype(jnp.float32) + added).astype(jnp.bfloat16)


def body(
    mixer_output_stream,
    layer_output_gradient,
    routes,
    expert_combine_weight,
    expert_gate_weight,
    expert_up_weight,
    expert_down_weight,
    head_mixer_input,
    head_step_size,
    head_decay_rate,
    extra_log_decay,
    state_entering_span,
    state_input_vectors,
    state_readout_vectors,
    gate_preactivation,
    group_norm_scale,
    mixer_output_weight,
):
    expert_count, me = lax.axis_size("sp"), lax.axis_index("sp")
    local_tokens = routes.shape[0]
    capacity = 3 * local_tokens // expert_count
    w_gate = expert_gate_weight[0]
    w_up = expert_up_weight[0]
    w_down = expert_down_weight[0]
    out_weight = lax.all_gather(mixer_output_weight, "sp", axis=1, tiled=True)
    select, slot_weight = pair_slots(routes ^ me, expert_combine_weight, expert_count, capacity)
    packed = pack_rows(mixer_output_stream, layer_output_gradient, select, slot_weight)
    packed = packed.reshape(expert_count, capacity, -1)
    received = exchange_relative([packed[m] for m in range(expert_count)], "sp")
    part_width = mixer_output_stream.shape[1]
    received = jnp.concatenate(received, axis=0)
    routed_rows = gather_columns(received[:, :part_width], "tp")
    routed_grads = gather_columns(received[:, part_width:], "tp")

    head_local = head_step_size.shape[1]
    group_local = state_input_vectors.shape[1] // STATE
    input_heads = head_mixer_input.astype(jnp.float32).reshape(local_tokens, head_local, HDIM)
    input_vector_groups = state_input_vectors.astype(jnp.float32).reshape(
        local_tokens, group_local, STATE
    )
    readout_groups = state_readout_vectors.astype(jnp.float32).reshape(
        local_tokens, group_local, STATE
    )
    within_span_state, within_span_log = span_final_state(
        input_heads, head_step_size, head_decay_rate, extra_log_decay, input_vector_groups
    )
    span_logs = gather_relative(within_span_log, "sp")
    carry_in, carry_log = state_before(within_span_state, span_logs, "sp")
    incoming_state = carry_in + scaled_by(carry_log, state_entering_span)

    def forward(input_values, time_step_values, input_vector_entries, readout_entries):
        return span_local_scan(
            input_values,
            time_step_values,
            head_decay_rate,
            extra_log_decay,
            input_vector_entries,
            readout_entries,
            incoming_state,
        )

    (scan_out, closing_state), pull_back = jax.vjp(
        forward, input_heads, head_step_size, input_vector_groups, readout_groups
    )

    def apply_norm(scan_vals, gate_vals):
        return gate_norm(scan_vals, gate_vals, group_norm_scale, group_local)

    normed, pull_norm = jax.vjp(apply_norm, scan_out, gate_preactivation.astype(jnp.float32))
    all_normed = lax.all_gather(normed.astype(jnp.bfloat16), "sp", axis=0, tiled=True)

    hidden, gate_grad, up_grad = expert_hidden(routed_rows, routed_grads, w_gate, w_up, w_down)
    partial_rows = row_partial(gate_grad, up_grad, w_gate, w_up)
    summed = scatter_sum_columns(partial_rows, "tp").reshape(expert_count, capacity, -1)
    returned = exchange_relative([summed[m] for m in range(expert_count)], "sp")
    own_cols = add_returns(layer_output_gradient, jnp.concatenate(returned, axis=0), select)
    grad_g, grad_u, grad_d = expert_weight_grads(
        routed_rows, routed_grads, hidden, gate_grad, up_grad
    )
    mix_grad = gather_columns(own_cols, "tp")
    out_width = mixer_output_weight.shape[1]
    normed_grad = lax.dot_general(
        mix_grad, out_weight, (((1,), (1,)), ((), ())), preferred_element_type=jnp.float32
    )
    mix_parts = exchange_relative(
        [
            lax.dynamic_slice_in_dim(mix_grad, (me ^ m) * out_width, out_width, axis=1)
            for m in range(expert_count)
        ],
        "sp",
    )
    scanned_gradient, gate_grad_in = pull_norm(normed_grad)
    reached_gradient = carried_weight(
        scanned_gradient, readout_groups, head_step_size, head_decay_rate, extra_log_decay
    )
    later_grad = state_after(reached_gradient, span_logs, "sp")
    input_grad, step_grad, b_grad, c_grad = pull_back((scanned_gradient, later_grad))
    all_mix = jnp.take(jnp.stack(mix_parts), me ^ jnp.arange(expert_count), axis=0)
    proj_grad = lax.dot_general(
        all_normed,
        all_mix.reshape(-1, out_width),
        (((0,), (0,)), ((), ())),
        preferred_element_type=jnp.float32,
    )
    return (
        grad_g[None],
        grad_u[None],
        grad_d[None],
        proj_grad,
        input_grad.reshape(local_tokens, -1).astype(jnp.bfloat16),
        step_grad,
        b_grad.reshape(local_tokens, -1).astype(jnp.bfloat16),
        c_grad.reshape(local_tokens, -1).astype(jnp.bfloat16),
        gate_grad_in.astype(jnp.bfloat16),
    )


def solution(mesh):
    return jax.shard_map(
        body,
        mesh=mesh,
        in_specs=(
            P("sp", "tp"),
            P("sp", "tp"),
            P("sp", None),
            P("sp", None),
            P("sp", None, "tp"),
            P("sp", None, "tp"),
            P("sp", "tp", None),
            P("sp", "tp"),
            P("sp", "tp"),
            P("tp"),
            P("sp", "tp"),
            P("tp", None, None),
            P("sp", "tp"),
            P("sp", "tp"),
            P("sp", "tp"),
            P("tp"),
            P("tp", "sp"),
        ),
        out_specs=(
            P("sp", None, "tp"),
            P("sp", None, "tp"),
            P("sp", "tp", None),
            P("tp", "sp"),
            P("sp", "tp"),
            P("sp", "tp"),
            P("sp", "tp"),
            P("sp", "tp"),
            P("sp", "tp"),
        ),
        check_vma=False,
    )
```

```python
import functools
import jax
import jax.numpy as jnp
from jax import lax
from jax.experimental import pallas as pl
from jax.experimental.pallas import tpu as pltpu
from jax.sharding import PartitionSpec as P


HDIM = 64
STATE = 128
LANES = 2 * HDIM

norm_eps = 1e-05
exact_mode = lax.Precision.HIGHEST
F32, BF16 = jnp.float32, jnp.bfloat16
NN = (((1,), (0,)), ((), ()))
NT = (((1,), (1,)), ((), ()))
TN = (((0,), (0,)), ((), ()))


def mm(a, b, kind):
    return lax.dot_general(a, b, kind, preferred_element_type=F32)


def exact(a, b, kind):
    return lax.dot_general(a, b, kind, precision=exact_mode, preferred_element_type=F32)


def iota(shape, dim):
    return lax.broadcasted_iota(jnp.int32, shape, dim)


def lower_half(rows):
    return iota((rows, LANES), 1) < HDIM


def spread(cols, q):
    return jnp.where(
        lower_half(cols.shape[0]), cols[:, 2 * q : 2 * q + 1], cols[:, 2 * q + 1 : 2 * q + 2]
    )


def put_halves(total, value, q):
    low = lower_half(value.shape[0])
    at = iota(total.shape, 1)
    first = jnp.sum(jnp.where(low, value, 0.0), axis=1, keepdims=True)
    second = jnp.sum(jnp.where(low, 0.0, value), axis=1, keepdims=True)
    total = jnp.where(at == 2 * q, total + first, total)
    return jnp.where(at == 2 * q + 1, total + second, total)


def pair(q):
    return slice(q * LANES, (q + 1) * LANES)


def group_cols(ref, g):
    return ref[:, g * STATE : (g + 1) * STATE]


def log_decay(dt_ref, rate_ref, extra_ref):
    return extra_ref[...] - dt_ref[...] * rate_ref[...]


def running_sums(logs):
    length = logs.shape[0]
    up_to = (iota((length, length), 0) >= iota((length, length), 1)).astype(F32)
    return exact(up_to, logs, NN), exact(logs, up_to, (((0,), (1,)), ((), ())))


def log_rows(logs):
    whole = exact(logs, jnp.ones((logs.shape[0], LANES), F32), TN)
    return packed_logs(whole)


def packed_logs(whole):
    high = whole.astype(BF16).astype(F32)
    return jnp.where(lower_half(whole.shape[0]), high, whole - high).astype(BF16)


def unpacked_logs(rows):
    rows = rows.astype(F32)
    return jnp.broadcast_to(rows[:, :1] + rows[:, HDIM : HDIM + 1], rows.shape)


def state_kernel(x_ref, dt_ref, rate_ref, extra_ref, b_ref, out_ref):
    logs = log_decay(dt_ref, rate_ref, extra_ref)
    cum, _ = running_sums(logs)
    weight = dt_ref[...] * jnp.exp(cum[-1:] - cum)
    pairs = x_ref.shape[1] // LANES
    each = pairs // (b_ref.shape[1] // STATE)
    for q in range(pairs):
        scaled = (x_ref[:, pair(q)].astype(F32) * spread(weight, q)).astype(BF16)
        out_ref[pair(q), :] = mm(scaled, group_cols(b_ref, q // each), TN).astype(BF16)
    out_ref[x_ref.shape[1] :, :] = log_rows(logs)


def join_kernel(first, last, forward, use_ref, own_ref, got_ref, *refs):
    refs = list(refs)
    width = refs[-1].shape[0] if last else refs[-2].shape[0]
    heads = width // HDIM
    use = use_ref[0, 0]
    mine = unpacked_logs(own_ref[width:, :])
    other = unpacked_logs(got_ref[width:, :])
    if first:
        scale = jnp.full(mine.shape, use)
        gap = use * other
    else:
        before_ref, gap_ref = refs.pop(0), refs.pop(0)
        scale = use * jnp.exp(gap_ref[...])
        gap = gap_ref[...] + use * other
    if last and forward:
        entering_ref = refs.pop(0)
        keep = jnp.exp(gap)
    if not last:
        total_ref, prefix_ref, gap_out_ref = refs
        gap_out_ref[...] = gap
        from_got, from_own = jnp.exp(use * mine), jnp.exp((1.0 - use) * other)
        total_ref[width:, :] = packed_logs(mine + other)
    else:
        (prefix_ref,) = refs
    for h in range(heads):
        rows = slice(h * HDIM, (h + 1) * HDIM)
        got = got_ref[rows, :].astype(F32)
        value = scale[h : h + 1] * got
        if not first:
            value = value + before_ref[rows, :]
        if last and forward:
            value = value + keep[h : h + 1] * entering_ref[rows, :]
        prefix_ref[rows, :] = value.astype(prefix_ref.dtype)
        if not last:
            own = own_ref[rows, :].astype(F32)
            total_ref[rows, :] = (
                from_got[h : h + 1] * got + from_own[h : h + 1] * own
            ).astype(BF16)


def scan_kernel(
    x_ref, dt_ref, rate_ref, extra_ref, b_ref, c_ref, in_ref, z_ref, gain_ref, y_ref, normed_ref
):
    cum, cum_t = running_sums(log_decay(dt_ref, rate_ref, extra_ref))
    grown = jnp.exp(cum)
    length = cum.shape[0]
    causal = iota((length, length), 0) >= iota((length, length), 1)
    dt = dt_ref[...]
    groups = b_ref.shape[1] // STATE
    pairs = x_ref.shape[1] // LANES
    each = pairs // groups
    for g in range(groups):
        b_g, c_g = group_cols(b_ref, g), group_cols(c_ref, g)
        affinity = mm(c_g, b_g, NT)
        for q in range(g * each, (g + 1) * each):
            scaled = (x_ref[:, pair(q)].astype(F32) * spread(dt, q)).astype(BF16)
            parts = []
            for h in (2 * q, 2 * q + 1):
                gaps = cum[:, h : h + 1] - cum_t[h : h + 1, :]
                decays = jnp.where(causal, jnp.exp(jnp.where(causal, gaps, 0.0)), 0.0)
                parts.append(mm((affinity * decays).astype(BF16), scaled, NN))
            inside = jnp.where(lower_half(length), parts[0], parts[1])
            carried = mm(c_g, in_ref[pair(q), :].astype(BF16), NT)
            y_ref[:, pair(q)] = inside + carried * spread(grown, q)
        cols = slice(g * each * LANES, (g + 1) * each * LANES)
        z = z_ref[:, cols].astype(F32)
        gated = y_ref[:, cols] * (z * jax.nn.sigmoid(z))
        factor = lax.rsqrt(jnp.mean(gated * gated, axis=1, keepdims=True) + norm_eps)
        normed_ref[:, cols] = (gated * factor * gain_ref[:, cols]).astype(BF16)


def norm_back_kernel(
    blocks, dt_ref, rate_ref, extra_ref, c_ref, y_ref, z_ref, gain_ref, mix_ref, *refs
):
    w_refs, (dy_ref, dz_ref, reach_ref) = refs[:blocks], refs[blocks:]
    logs = log_decay(dt_ref, rate_ref, extra_ref)
    cum, _ = running_sums(logs)
    grown = jnp.exp(cum)
    groups = c_ref.shape[1] // STATE
    pairs = y_ref.shape[1] // LANES
    each = pairs // groups
    for g in range(groups):
        cols = slice(g * each * LANES, (g + 1) * each * LANES)
        up = mm(mix_ref[0], w_refs[0][cols, :], NT)
        for m in range(1, blocks):
            up = up + mm(mix_ref[m], w_refs[m][cols, :], NT)
        up = up * gain_ref[:, cols]
        z, y = z_ref[:, cols].astype(F32), y_ref[:, cols]
        sig = jax.nn.sigmoid(z)
        gated = y * (z * sig)
        factor = lax.rsqrt(jnp.mean(gated * gated, axis=1, keepdims=True) + norm_eps)
        shared = jnp.mean(up * gated, axis=1, keepdims=True) * factor * factor
        d_gated = factor * (up - gated * shared)
        dy_ref[:, cols] = (d_gated * (z * sig)).astype(BF16)
        dz_ref[:, cols] = (d_gated * y * sig * (1.0 + z * (1.0 - sig))).astype(BF16)
        c_g = group_cols(c_ref, g)
        for q in range(g * each, (g + 1) * each):
            weighted = (dy_ref[:, pair(q)].astype(F32) * spread(grown, q)).astype(BF16)
            reach_ref[pair(q), :] = mm(weighted, c_g, TN).astype(BF16)
    reach_ref[y_ref.shape[1] :, :] = log_rows(logs)


def inner_back_kernel(
    x_ref,
    dt_ref,
    rate_ref,
    extra_ref,
    b_ref,
    c_ref,
    in_ref,
    dy_ref,
    dx_ref,
    dc_ref,
    db_ref,
    at_ref,
    at_t_ref,
):
    cum, cum_t = running_sums(log_decay(dt_ref, rate_ref, extra_ref))
    grown = jnp.exp(cum)
    length = cum.shape[0]
    dt = dt_ref[...]
    later = iota((length, length), 1) >= iota((length, length), 0)
    low = lower_half(length)
    groups = b_ref.shape[1] // STATE
    pairs = x_ref.shape[1] // LANES
    each = pairs // groups
    at = jnp.zeros(cum.shape, F32)
    for g in range(groups):
        b_g, c_g = group_cols(b_ref, g), group_cols(c_ref, g)
        affinity = mm(b_g, c_g, NT)
        d_affinity = jnp.zeros((length, length), F32)
        dc = jnp.zeros((length, STATE), F32)
        for q in range(g * each, (g + 1) * each):
            scaled = (x_ref[:, pair(q)].astype(F32) * spread(dt, q)).astype(BF16)
            dy = dy_ref[:, pair(q)]
            parts = []
            for h in (2 * q, 2 * q + 1):
                gaps = cum_t[h : h + 1, :] - cum[:, h : h + 1]
                decays = jnp.where(later, jnp.exp(jnp.where(later, gaps, 0.0)), 0.0)
                half = jnp.where(low == (h % 2 == 0), scaled, jnp.zeros_like(scaled))
                back = mm(half, dy, NT)
                mixed = affinity * decays
                parts.append(mm(mixed.astype(BF16), dy, NN))
                moved = mixed * back
                d_affinity = d_affinity + decays * back
                lost = jnp.sum(moved, axis=1, keepdims=True)
                at = jnp.where(iota(at.shape, 1) == h, at - lost, at)
                at_t_ref[h : h + 1, :] = jnp.sum(moved, axis=0, keepdims=True)
            dx_ref[:, pair(q)] = jnp.where(low, parts[0], parts[1])
            held = in_ref[pair(q), :].astype(BF16)
            weighted = dy.astype(F32) * spread(grown, q)
            at = put_halves(at, weighted * mm(c_g, held, NT), q)
            dc = dc + mm(weighted.astype(BF16), held, NN)
        cols = slice(g * STATE, (g + 1) * STATE)
        d_affinity = d_affinity.astype(BF16)
        db_ref[:, cols] = mm(d_affinity, c_g, NN)
        dc_ref[:, cols] = (dc + mm(d_affinity, b_g, TN)).astype(BF16)
    at_ref[...] = at


def last_back_kernel(
    x_ref,
    dt_ref,
    rate_ref,
    extra_ref,
    b_ref,
    in_ref,
    later_ref,
    dx_ref,
    db_part_ref,
    at_ref,
    at_t_ref,
    d_input_ref,
    d_step_ref,
    db_ref,
):
    cum, _ = running_sums(log_decay(dt_ref, rate_ref, extra_ref))
    length, heads = cum.shape
    dt = dt_ref[...]
    to_end = jnp.exp(cum[-1:] - cum)
    groups = b_ref.shape[1] // STATE
    pairs = x_ref.shape[1] // LANES
    each = pairs // groups
    lost = jnp.zeros(cum.shape, F32)
    direct = jnp.zeros(cum.shape, F32)
    tail = jnp.zeros((1, heads), F32)
    for g in range(groups):
        b_g = group_cols(b_ref, g)
        db = db_part_ref[:, g * STATE : (g + 1) * STATE]
        for q in range(g * each, (g + 1) * each):
            grad = later_ref[pair(q), :]
            x = x_ref[:, pair(q)].astype(F32)
            scale = spread(dt, q)
            ending = spread(to_end, q)
            scaled = x * scale
            low_grad = grad.astype(BF16)
            dx_state = mm(b_g, low_grad, NT) * ending
            lost = put_halves(lost, scaled * dx_state, q)
            db = db + mm((scaled * ending).astype(BF16), low_grad, NN)
            dx = dx_ref[:, pair(q)] + dx_state
            d_input_ref[:, pair(q)] = (dx * scale).astype(BF16)
            direct = put_halves(direct, dx * x, q)
            kept = grad * in_ref[pair(q), :]
            for side in range(2):
                part = jnp.sum(kept[side * HDIM : (side + 1) * HDIM], axis=0, keepdims=True)
                part = jnp.sum(part, axis=1, keepdims=True)
                tail = jnp.where(iota(tail.shape, 1) == 2 * q + side, part, tail)
        db_ref[:, g * STATE : (g + 1) * STATE] = db.astype(BF16)
    from_here = (iota((length, length), 1) >= iota((length, length), 0)).astype(F32)
    d_log = exact(from_here, at_ref[...] - lost, NN) + exact(from_here, at_t_ref[...], NT)
    d_log = d_log + jnp.sum(lost, axis=0, keepdims=True) + jnp.exp(cum[-1:]) * tail
    d_step_ref[...] = (direct - d_log * rate_ref[...]).T


def call(kernel, outs, *args, scalars=0, name="kernel"):
    vmem, smem = pl.BlockSpec(memory_space=pltpu.VMEM), pl.BlockSpec(memory_space=pltpu.SMEM)
    return pl.pallas_call(
        kernel,
        out_shape=[jax.ShapeDtypeStruct(shape, kind) for shape, kind in outs],
        in_specs=[smem] * scalars + [vmem] * (len(args) - scalars),
        out_specs=[vmem] * len(outs),
        compiler_params=pltpu.CompilerParams(vmem_limit_bytes=(24 if name == "normback" else 12) << 20),
    )(*args)


def swapped(x, axis, mask):
    n = lax.axis_size(axis)
    return lax.ppermute(x, axis, [(i, i ^ mask) for i in range(n)])


def bits_of(n):
    return [1 << k for k in range(n.bit_length() - 1)]


def reorder(blocks, me, n):
    blocks = list(blocks)
    for bit in bits_of(n):
        is_set = (me & bit) != 0
        for m in range(n):
            if not m & bit:
                a, b = blocks[m], blocks[m | bit]
                blocks[m], blocks[m | bit] = jnp.where(is_set, b, a), jnp.where(is_set, a, b)
    return blocks


def gather_relative(x, axis):
    n = lax.axis_size(axis)
    blocks = {0: x}
    for bit in reversed(bits_of(n)):
        for m in sorted(blocks):
            blocks[m | bit] = swapped(blocks[m], axis, bit)
    return [blocks[m] for m in range(n)]


def exchange_relative(blocks, axis):
    swaps = [swapped(blocks[m], axis, m) for m in range(1, len(blocks))]
    return [blocks[0]] + swaps


def partner_kernel(width, spots, at_ref, x_ref, *refs):
    got_refs, out_ref = refs[:-1], refs[-1]
    for k in range(out_ref.shape[1] // width):
        start = pl.multiple_of(at_ref[0, k] * width, width)
        total = x_ref[:, pl.ds(start, width)].astype(F32)
        for got_ref, spot in zip(got_refs, spots):
            total = total + got_ref[:, spot[k] * width : (spot[k] + 1) * width].astype(F32)
        out_ref[:, k * width : (k + 1) * width] = total.astype(BF16)


def scatter_sum_columns(x, axis):
    n, me = lax.axis_size(axis), lax.axis_index(axis)
    width = x.shape[1] // n
    held, received = list(range(n)), []
    for bit in bits_of(n) + [0]:
        going = [m for m in held if m & bit] if bit else held
        spots = [[order.index(m) for m in going] for _, order in received]
        (sent,) = call(
            functools.partial(partner_kernel, width, spots),
            [((x.shape[0], width * len(going)), BF16)],
            jnp.stack([me ^ m for m in going]).astype(jnp.int32).reshape(1, -1),
            x,
            *[got for got, _ in received],
            scalars=1,
            name="sum",
        )
        if not bit:
            return sent
        held = [m for m in held if not m & bit]
        received.append((swapped(sent, axis, bit), held))


def exchange_steps(held, sent, axis, events):
    parts, sources = [held], [0]
    for bit in reversed(bits_of(held.shape[0])):
        if len(parts) > 1:
            rows = [part.reshape(-1, *part.shape[-3:])[:, bit : 2 * bit] for part in parts]
            sent = jnp.concatenate(rows, axis=0)
        got = swapped(sent, axis, bit)
        parts.append(after(got, events[len(parts) - 1]) if len(parts) <= len(events) else got)
        sources += [source | bit for source in sources]
    return parts, sources


def gather_steps(x, axis, moved):
    n = lax.axis_size(axis)
    offsets, blocks = [0], [x]
    for bit in reversed(bits_of(n)):
        for m, block in list(zip(offsets, blocks)):
            hop = bit
            if m in moved:
                hop = moved[m]
                block = blocks[offsets.index(m ^ hop ^ bit)]
            blocks.append(swapped(block, axis, hop))
            offsets.append(m | bit)
    return offsets, blocks


def after(x, *events):
    return lax.optimization_barrier((x, *events))[0]


def spread_states(own, widths, entering, forward, axis, name, seen=None):
    width, heads = widths
    n, me = lax.axis_size(axis), lax.axis_index(axis)
    bits = bits_of(n)
    state = []
    for step, bit in enumerate(bits):
        first, last = step == 0, bit == bits[-1]
        uses = ((me & bit) != 0) == forward
        use = jnp.where(uses, 1.0, 0.0).astype(F32).reshape(1, 1)
        args = [use, own, swapped(own, axis, bit)] + state
        outs = [((width, STATE), F32)]
        if last and forward:
            args.append(entering)
        if not last:
            outs = [(own.shape, BF16)] + outs + [((heads, LANES), F32)]
        made = call(functools.partial(join_kernel, first, last, forward), outs, *args, scalars=1, name=name + ("last" if last else "join"))
        if last:
            return made[0]
        own, state = made[0], list(made[1:])
        if seen is not None:
            seen.append(own)


def return_kernel(grad_ref, select_ref, *refs):
    blocks, out_ref = refs[:-1], refs[-1]
    total = grad_ref[...].astype(F32)
    for m, block in enumerate(blocks):
        total = total + mm(select_ref[m], block[...], TN)
    out_ref[...] = total.astype(BF16)


def proj_kernel(places, *refs):
    refs, out_ref = refs[:-1], refs[-1]
    normed, mixes = refs[: len(places)], refs[len(places) :]
    chunk = 2 * LANES
    rows = [mixes[0][0]]
    for mix in mixes[1:]:
        shape = mix.shape
        sources = shape[0] if len(shape) == 4 else 1
        rows += [mix[k, 0] if len(shape) == 4 else mix[0] for k in range(sources)]
    for c in range(0, out_ref.shape[0], chunk):
        total = jnp.zeros((chunk, out_ref.shape[1]), F32)
        for place, row in zip(places, rows):
            total = total + mm(normed[place][:, c : c + chunk], row, TN)
        out_ref[c : c + chunk, :] = total


def mix_kernel(place_ref, *refs):
    blocks, (mix_ref, sent_ref) = refs[:-2], refs[-2:]
    count, _, width = mix_ref.shape
    each = count // len(blocks)
    for m, block in enumerate(blocks):
        for part in range(each):
            at = place_ref[0, m * each + part]
            mix_ref[at] = block[:, part * width : (part + 1) * width]

            @pl.when(at >= count // 2)
            def _():
                sent_ref[at - count // 2] = block[:, part * width : (part + 1) * width]


def pack_kernel(experts, routes_ref, weight_ref, x_ref, grad_ref, packed_ref, select_ref):
    slots, tokens = select_ref.shape
    capacity = slots // experts
    width = x_ref.shape[1]
    numbers = iota((experts, tokens), 0)
    mask = jnp.zeros((experts, tokens), F32)
    weight = jnp.zeros((experts, tokens), F32)
    for k in range(routes_ref.shape[0]):
        chosen = routes_ref[k : k + 1, :] == numbers
        mask = jnp.where(chosen, 1.0, mask)
        weight = jnp.where(chosen, weight_ref[k : k + 1, :], weight)
    earlier = (iota((tokens, tokens), 0) < iota((tokens, tokens), 1)).astype(BF16)
    place = jnp.where(mask > 0.5, mm(mask.astype(BF16), earlier, NN), -1.0)
    row, number = iota((slots, experts), 0), iota((slots, experts), 1) * capacity
    owner = jnp.logical_and(row >= number, row < number + capacity).astype(F32)
    first = jnp.sum(owner * number.astype(F32), axis=1, keepdims=True)
    at_row = mm(owner.astype(BF16), place.astype(BF16), NN)
    at_slot = at_row + first == iota((slots, tokens), 0).astype(F32)
    at_slot = jnp.logical_and(at_slot, at_row > -0.5)
    of_row = exact(owner, weight, NN)
    slot_weight = jnp.sum(jnp.where(at_slot, of_row, 0.0), axis=1, keepdims=True)
    select = at_slot.astype(BF16)
    select_ref[...] = select
    packed_ref[:, :width] = mm(select, x_ref[...], NN).astype(BF16)
    packed_ref[:, width:] = (mm(select, grad_ref[...], NN) * slot_weight).astype(BF16)


def expert_hidden(routed_rows, routed_grads, w_gate, w_up, w_down):
    pre_gate = jnp.dot(routed_rows, w_gate, preferred_element_type=jnp.float32)
    pre_up = jnp.dot(routed_rows, w_up, preferred_element_type=jnp.float32)
    activated = jax.nn.silu(pre_gate)
    hidden = (activated * pre_up).astype(jnp.bfloat16)
    hidden_grad = lax.dot_general(
        routed_grads, w_down, (((1,), (1,)), ((), ())), preferred_element_type=jnp.float32
    )
    sigmoid_gate = jax.nn.sigmoid(pre_gate)
    gate_grad = (
        hidden_grad * pre_up * sigmoid_gate * (1.0 + pre_gate * (1.0 - sigmoid_gate))
    ).astype(jnp.bfloat16)
    up_grad = (hidden_grad * activated).astype(jnp.bfloat16)
    return (hidden, gate_grad, up_grad)


def expert_weight_grads(routed_rows, routed_grads, hidden, gate_grad, up_grad):
    contract = (((0,), (0,)), ((), ()))
    grad_g = lax.dot_general(routed_rows, gate_grad, contract, preferred_element_type=jnp.float32)
    grad_u = lax.dot_general(routed_rows, up_grad, contract, preferred_element_type=jnp.float32)
    grad_d = lax.dot_general(hidden, routed_grads, contract, preferred_element_type=jnp.float32)
    return (grad_g.astype(jnp.bfloat16), grad_u.astype(jnp.bfloat16), grad_d.astype(jnp.bfloat16))


def row_partial(gate_grad, up_grad, w_gate, w_up):
    contract = (((1,), (1,)), ((), ()))
    partial_sum = lax.dot_general(gate_grad, w_gate, contract, preferred_element_type=jnp.float32)
    partial_sum = partial_sum + lax.dot_general(
        up_grad, w_up, contract, preferred_element_type=jnp.float32
    )
    return partial_sum.astype(jnp.bfloat16)


def body(
    mixer_output_stream,
    layer_output_gradient,
    routes,
    expert_combine_weight,
    expert_gate_weight,
    expert_up_weight,
    expert_down_weight,
    head_mixer_input,
    head_step_size,
    head_decay_rate,
    extra_log_decay,
    state_entering_span,
    state_input_vectors,
    state_readout_vectors,
    gate_preactivation,
    group_norm_scale,
    mixer_output_weight,
):
    expert_count, me = lax.axis_size("sp"), lax.axis_index("sp")
    local_tokens, heads = head_step_size.shape
    width = head_mixer_input.shape[1]
    vectors = state_input_vectors.shape[1]
    capacity = 3 * local_tokens // expert_count
    w_gate = expert_gate_weight[0]
    w_up = expert_up_weight[0]
    w_down = expert_down_weight[0]
    rate = head_decay_rate[None, :]
    gain = group_norm_scale[None, :]
    entering = state_entering_span.reshape(width, STATE)

    slots = expert_count * capacity
    packed, select = call(
        functools.partial(pack_kernel, expert_count),
        [((slots, 2 * mixer_output_stream.shape[1]), BF16), ((slots, local_tokens), BF16)],
        routes.T ^ me,
        expert_combine_weight.T,
        mixer_output_stream,
        layer_output_gradient,
        name="pack",
    )
    packed, step_size = lax.optimization_barrier((packed, head_step_size))
    scan_args = (head_mixer_input, step_size, rate, extra_log_decay)
    rows = packed.reshape(expert_count, capacity, -1)
    received = exchange_relative([rows[m] for m in range(expert_count)], "sp")
    received = jnp.concatenate(received, axis=0)

    (own_state,) = call(
        state_kernel, [((width + heads, STATE), BF16)], *scan_args, state_input_vectors
    )
    part_width = mixer_output_stream.shape[1]
    gathered = gather_relative(received, "tp")
    gathered = reorder(gathered, lax.axis_index("tp"), lax.axis_size("tp"))
    routed_rows = jnp.concatenate([part[:, :part_width] for part in gathered], axis=1)
    routed_grads = jnp.concatenate([part[:, part_width:] for part in gathered], axis=1)
    hidden, gate_grad, up_grad = expert_hidden(routed_rows, routed_grads, w_gate, w_up, w_down)
    partial_rows = row_partial(gate_grad, up_grad, w_gate, w_up)
    summed = scatter_sum_columns(partial_rows, "tp")
    offsets, weights = gather_steps(after(mixer_output_weight, received), "sp", {})
    incoming = spread_states(
        own_state, (width, heads), entering, True, "sp", "f"
    )
    scan_out, normed = call(
        scan_kernel,
        [((local_tokens, width), F32), ((local_tokens, width), BF16)],
        *scan_args,
        state_input_vectors,
        state_readout_vectors,
        after(incoming, summed),
        gate_preactivation,
        gain,
    )
    summed = summed.reshape(expert_count, capacity, -1)
    returned = exchange_relative([summed[m] for m in range(expert_count)], "sp")
    (own_cols,) = call(
        return_kernel,
        [(layer_output_gradient.shape, BF16)],
        layer_output_gradient,
        select.reshape(expert_count, capacity, local_tokens),
        *returned,
        name="back",
    )
    grad_g, grad_u, grad_d = expert_weight_grads(
        routed_rows, routed_grads, hidden, gate_grad, up_grad
    )
    own_parts = gather_relative(own_cols, "tp")
    out_width = mixer_output_weight.shape[1]
    each = part_width // out_width
    numbers = jnp.arange(expert_count, dtype=jnp.int32)
    place = me ^ (((numbers // each) ^ lax.axis_index("tp")) * each + numbers % each)
    mix_parts, mix_sent = call(
        mix_kernel,
        [
            ((expert_count, local_tokens, out_width), BF16),
            ((expert_count // 2, local_tokens, out_width), BF16),
        ],
        place.reshape(1, -1),
        *own_parts,
        scalars=1,
        name="mix",
    )

    scan_grad, gate_grad_in, reached = call(
        functools.partial(norm_back_kernel, expert_count),
        [((local_tokens, width), BF16)] * 2 + [((width + heads, STATE), BF16)],
        *scan_args[1:],
        state_readout_vectors,
        scan_out,
        gate_preactivation,
        gain,
        mix_parts,
        *[weights[offsets.index(m)] for m in range(expert_count)],
        name="normback",
    )
    joined = []
    later = spread_states(reached, (width, heads), None, False, "sp", "b", joined)
    inner_x_grad, c_grad, inner_b_grad, at, at_t = call(
        inner_back_kernel,
        [
            ((local_tokens, width), F32),
            ((local_tokens, vectors), BF16),
            ((local_tokens, vectors), F32),
            ((local_tokens, heads), F32),
            ((heads, local_tokens), F32),
        ],
        *scan_args,
        state_input_vectors,
        state_readout_vectors,
        incoming,
        scan_grad,
        name="inner",
    )
    kept, all_normed = gather_steps(normed, "sp", {6: 2})
    all_mix, sources = exchange_steps(mix_parts, mix_sent, "sp", (grad_d, grad_u))
    input_grad, step_grad, b_grad = call(
        last_back_kernel,
        [
            ((local_tokens, width), BF16),
            ((heads, local_tokens), F32),
            ((local_tokens, vectors), BF16),
        ],
        *scan_args,
        state_input_vectors,
        incoming,
        later,
        inner_x_grad,
        inner_b_grad,
        at,
        at_t,
    )
    all_normed[-1] = after(all_normed[-1], step_grad)
    (proj_grad,) = call(
        functools.partial(proj_kernel, [kept.index(m) for m in sources]),
        [((width, out_width), F32)],
        *all_normed,
        *all_mix,
        name="proj",
    )
    return (
        grad_g[None],
        grad_u[None],
        grad_d[None],
        proj_grad,
        input_grad,
        step_grad.T,
        b_grad,
        c_grad,
        gate_grad_in,
    )


def solution(mesh):
    return jax.shard_map(
        body,
        mesh=mesh,
        in_specs=(
            P("sp", "tp"),
            P("sp", "tp"),
            P("sp", None),
            P("sp", None),
            P("sp", None, "tp"),
            P("sp", None, "tp"),
            P("sp", "tp", None),
            P("sp", "tp"),
            P("sp", "tp"),
            P("tp"),
            P("sp", "tp"),
            P("tp", None, None),
            P("sp", "tp"),
            P("sp", "tp"),
            P("sp", "tp"),
            P("tp"),
            P("tp", "sp"),
        ),
        out_specs=(
            P("sp", None, "tp"),
            P("sp", None, "tp"),
            P("sp", "tp", None),
            P("tp", "sp"),
            P("sp", "tp"),
            P("sp", "tp"),
            P("sp", "tp"),
            P("sp", "tp"),
            P("sp", "tp"),
        ),
        check_vma=False,
    )
```

```python
import functools
import jax
import jax.numpy as jnp
from jax import lax
from jax.experimental import pallas as pl
from jax.experimental.pallas import tpu as pltpu
from jax.sharding import PartitionSpec as P


HDIM = 64
STATE = 128
LANES = 2 * HDIM

norm_eps = 1e-05
exact_mode = lax.Precision.HIGHEST
F32, BF16 = jnp.float32, jnp.bfloat16
NN = (((1,), (0,)), ((), ()))
NT = (((1,), (1,)), ((), ()))
TN = (((0,), (0,)), ((), ()))


def mm(a, b, kind):
    return lax.dot_general(a, b, kind, preferred_element_type=F32)


def exact(a, b, kind):
    return lax.dot_general(a, b, kind, precision=exact_mode, preferred_element_type=F32)


def iota(shape, dim):
    return lax.broadcasted_iota(jnp.int32, shape, dim)


def lower_half(rows):
    return iota((rows, LANES), 1) < HDIM


def spread(cols, q):
    return jnp.where(
        lower_half(cols.shape[0]), cols[:, 2 * q : 2 * q + 1], cols[:, 2 * q + 1 : 2 * q + 2]
    )


def put_halves(total, value, q):
    low = lower_half(value.shape[0])
    at = iota(total.shape, 1)
    first = jnp.sum(jnp.where(low, value, 0.0), axis=1, keepdims=True)
    second = jnp.sum(jnp.where(low, 0.0, value), axis=1, keepdims=True)
    total = jnp.where(at == 2 * q, total + first, total)
    return jnp.where(at == 2 * q + 1, total + second, total)


def pair(q):
    return slice(q * LANES, (q + 1) * LANES)


def group_cols(ref, g):
    return ref[:, g * STATE : (g + 1) * STATE]


def log_decay(dt_ref, rate_ref, extra_ref):
    return extra_ref[...] - dt_ref[...] * rate_ref[...]


def running_sums(logs):
    length = logs.shape[0]
    up_to = (iota((length, length), 0) >= iota((length, length), 1)).astype(F32)
    return exact(up_to, logs, NN), exact(logs, up_to, (((0,), (1,)), ((), ())))


def log_rows(logs):
    whole = exact(logs, jnp.ones((logs.shape[0], LANES), F32), TN)
    return packed_logs(whole)


def packed_logs(whole):
    high = whole.astype(BF16).astype(F32)
    return jnp.where(lower_half(whole.shape[0]), high, whole - high).astype(BF16)


def unpacked_logs(rows):
    rows = rows.astype(F32)
    return jnp.broadcast_to(rows[:, :1] + rows[:, HDIM : HDIM + 1], rows.shape)


def state_kernel(x_ref, dt_ref, rate_ref, extra_ref, b_ref, out_ref):
    logs = log_decay(dt_ref, rate_ref, extra_ref)
    cum, _ = running_sums(logs)
    weight = dt_ref[...] * jnp.exp(cum[-1:] - cum)
    pairs = x_ref.shape[1] // LANES
    each = pairs // (b_ref.shape[1] // STATE)
    for q in range(pairs):
        scaled = (x_ref[:, pair(q)].astype(F32) * spread(weight, q)).astype(BF16)
        out_ref[pair(q), :] = mm(scaled, group_cols(b_ref, q // each), TN).astype(BF16)
    out_ref[x_ref.shape[1] :, :] = log_rows(logs)


def join_kernel(first, last, forward, use_ref, own_ref, got_ref, *refs):
    refs = list(refs)
    width = refs[-1].shape[0] if last else refs[-2].shape[0]
    heads = width // HDIM
    use = use_ref[0, 0]
    mine = unpacked_logs(own_ref[width:, :])
    other = unpacked_logs(got_ref[width:, :])
    if first:
        scale = jnp.full(mine.shape, use)
        gap = use * other
    else:
        before_ref, gap_ref = refs.pop(0), refs.pop(0)
        scale = use * jnp.exp(gap_ref[...])
        gap = gap_ref[...] + use * other
    if last and forward:
        entering_ref = refs.pop(0)
        keep = jnp.exp(gap)
    if not last:
        total_ref, prefix_ref, gap_out_ref = refs
        gap_out_ref[...] = gap
        from_got, from_own = jnp.exp(use * mine), jnp.exp((1.0 - use) * other)
        total_ref[width:, :] = packed_logs(mine + other)
    else:
        (prefix_ref,) = refs
    for h in range(heads):
        rows = slice(h * HDIM, (h + 1) * HDIM)
        got = got_ref[rows, :].astype(F32)
        value = scale[h : h + 1] * got
        if not first:
            value = value + before_ref[rows, :]
        if last and forward:
            value = value + keep[h : h + 1] * entering_ref[rows, :]
        prefix_ref[rows, :] = value.astype(prefix_ref.dtype)
        if not last:
            own = own_ref[rows, :].astype(F32)
            total_ref[rows, :] = (
                from_got[h : h + 1] * got + from_own[h : h + 1] * own
            ).astype(BF16)


def scan_kernel(
    x_ref, dt_ref, rate_ref, extra_ref, b_ref, c_ref, in_ref, z_ref, gain_ref, y_ref, normed_ref
):
    cum, cum_t = running_sums(log_decay(dt_ref, rate_ref, extra_ref))
    grown = jnp.exp(cum)
    length = cum.shape[0]
    causal = iota((length, length), 0) >= iota((length, length), 1)
    dt = dt_ref[...]
    groups = b_ref.shape[1] // STATE
    pairs = x_ref.shape[1] // LANES
    each = pairs // groups
    for g in range(groups):
        b_g, c_g = group_cols(b_ref, g), group_cols(c_ref, g)
        affinity = mm(c_g, b_g, NT)
        for q in range(g * each, (g + 1) * each):
            scaled = (x_ref[:, pair(q)].astype(F32) * spread(dt, q)).astype(BF16)
            parts = []
            for h in (2 * q, 2 * q + 1):
                gaps = cum[:, h : h + 1] - cum_t[h : h + 1, :]
                decays = jnp.where(causal, jnp.exp(jnp.where(causal, gaps, 0.0)), 0.0)
                parts.append(mm((affinity * decays).astype(BF16), scaled, NN))
            inside = jnp.where(lower_half(length), parts[0], parts[1])
            carried = mm(c_g, in_ref[pair(q), :].astype(BF16), NT)
            y_ref[:, pair(q)] = inside + carried * spread(grown, q)
        cols = slice(g * each * LANES, (g + 1) * each * LANES)
        z = z_ref[:, cols].astype(F32)
        gated = y_ref[:, cols] * (z * jax.nn.sigmoid(z))
        factor = lax.rsqrt(jnp.mean(gated * gated, axis=1, keepdims=True) + norm_eps)
        normed_ref[:, cols] = (gated * factor * gain_ref[:, cols]).astype(BF16)


def norm_back_kernel(
    blocks, dt_ref, rate_ref, extra_ref, c_ref, y_ref, z_ref, gain_ref, mix_ref, *refs
):
    w_refs, (dy_ref, dz_ref, reach_ref) = refs[:blocks], refs[blocks:]
    logs = log_decay(dt_ref, rate_ref, extra_ref)
    cum, _ = running_sums(logs)
    grown = jnp.exp(cum)
    groups = c_ref.shape[1] // STATE
    pairs = y_ref.shape[1] // LANES
    each = pairs // groups
    for g in range(groups):
        cols = slice(g * each * LANES, (g + 1) * each * LANES)
        up = mm(mix_ref[0], w_refs[0][cols, :], NT)
        for m in range(1, blocks):
            up = up + mm(mix_ref[m], w_refs[m][cols, :], NT)
        up = up * gain_ref[:, cols]
        z, y = z_ref[:, cols].astype(F32), y_ref[:, cols]
        sig = jax.nn.sigmoid(z)
        gated = y * (z * sig)
        factor = lax.rsqrt(jnp.mean(gated * gated, axis=1, keepdims=True) + norm_eps)
        shared = jnp.mean(up * gated, axis=1, keepdims=True) * factor * factor
        d_gated = factor * (up - gated * shared)
        dy_ref[:, cols] = (d_gated * (z * sig)).astype(BF16)
        dz_ref[:, cols] = (d_gated * y * sig * (1.0 + z * (1.0 - sig))).astype(BF16)
        c_g = group_cols(c_ref, g)
        for q in range(g * each, (g + 1) * each):
            weighted = (dy_ref[:, pair(q)].astype(F32) * spread(grown, q)).astype(BF16)
            reach_ref[pair(q), :] = mm(weighted, c_g, TN).astype(BF16)
    reach_ref[y_ref.shape[1] :, :] = log_rows(logs)


def inner_back_kernel(
    x_ref,
    dt_ref,
    rate_ref,
    extra_ref,
    b_ref,
    c_ref,
    in_ref,
    dy_ref,
    dx_ref,
    dc_ref,
    db_ref,
    at_ref,
    at_t_ref,
):
    cum, cum_t = running_sums(log_decay(dt_ref, rate_ref, extra_ref))
    grown = jnp.exp(cum)
    length = cum.shape[0]
    dt = dt_ref[...]
    later = iota((length, length), 1) >= iota((length, length), 0)
    low = lower_half(length)
    groups = b_ref.shape[1] // STATE
    pairs = x_ref.shape[1] // LANES
    each = pairs // groups
    at = jnp.zeros(cum.shape, F32)
    for g in range(groups):
        b_g, c_g = group_cols(b_ref, g), group_cols(c_ref, g)
        affinity = mm(b_g, c_g, NT)
        d_affinity = jnp.zeros((length, length), F32)
        dc = jnp.zeros((length, STATE), F32)
        for q in range(g * each, (g + 1) * each):
            scaled = (x_ref[:, pair(q)].astype(F32) * spread(dt, q)).astype(BF16)
            dy = dy_ref[:, pair(q)]
            parts = []
            for h in (2 * q, 2 * q + 1):
                gaps = cum_t[h : h + 1, :] - cum[:, h : h + 1]
                decays = jnp.where(later, jnp.exp(jnp.where(later, gaps, 0.0)), 0.0)
                half = jnp.where(low == (h % 2 == 0), scaled, jnp.zeros_like(scaled))
                back = mm(half, dy, NT)
                mixed = affinity * decays
                parts.append(mm(mixed.astype(BF16), dy, NN))
                moved = mixed * back
                d_affinity = d_affinity + decays * back
                lost = jnp.sum(moved, axis=1, keepdims=True)
                at = jnp.where(iota(at.shape, 1) == h, at - lost, at)
                at_t_ref[h : h + 1, :] = jnp.sum(moved, axis=0, keepdims=True)
            dx_ref[:, pair(q)] = jnp.where(low, parts[0], parts[1])
            held = in_ref[pair(q), :].astype(BF16)
            weighted = dy.astype(F32) * spread(grown, q)
            at = put_halves(at, weighted * mm(c_g, held, NT), q)
            dc = dc + mm(weighted.astype(BF16), held, NN)
        cols = slice(g * STATE, (g + 1) * STATE)
        d_affinity = d_affinity.astype(BF16)
        db_ref[:, cols] = mm(d_affinity, c_g, NN)
        dc_ref[:, cols] = (dc + mm(d_affinity, b_g, TN)).astype(BF16)
    at_ref[...] = at


def last_back_kernel(
    x_ref,
    dt_ref,
    rate_ref,
    extra_ref,
    b_ref,
    in_ref,
    later_ref,
    dx_ref,
    db_part_ref,
    at_ref,
    at_t_ref,
    d_input_ref,
    d_step_ref,
    db_ref,
):
    cum, _ = running_sums(log_decay(dt_ref, rate_ref, extra_ref))
    length, heads = cum.shape
    dt = dt_ref[...]
    to_end = jnp.exp(cum[-1:] - cum)
    groups = b_ref.shape[1] // STATE
    pairs = x_ref.shape[1] // LANES
    each = pairs // groups
    lost = jnp.zeros(cum.shape, F32)
    direct = jnp.zeros(cum.shape, F32)
    tail = jnp.zeros((1, heads), F32)
    for g in range(groups):
        b_g = group_cols(b_ref, g)
        db = db_part_ref[:, g * STATE : (g + 1) * STATE]
        for q in range(g * each, (g + 1) * each):
            grad = later_ref[pair(q), :]
            x = x_ref[:, pair(q)].astype(F32)
            scale = spread(dt, q)
            ending = spread(to_end, q)
            scaled = x * scale
            low_grad = grad.astype(BF16)
            dx_state = mm(b_g, low_grad, NT) * ending
            lost = put_halves(lost, scaled * dx_state, q)
            db = db + mm((scaled * ending).astype(BF16), low_grad, NN)
            dx = dx_ref[:, pair(q)] + dx_state
            d_input_ref[:, pair(q)] = (dx * scale).astype(BF16)
            direct = put_halves(direct, dx * x, q)
            kept = grad * in_ref[pair(q), :]
            for side in range(2):
                part = jnp.sum(kept[side * HDIM : (side + 1) * HDIM], axis=0, keepdims=True)
                part = jnp.sum(part, axis=1, keepdims=True)
                tail = jnp.where(iota(tail.shape, 1) == 2 * q + side, part, tail)
        db_ref[:, g * STATE : (g + 1) * STATE] = db.astype(BF16)
    from_here = (iota((length, length), 1) >= iota((length, length), 0)).astype(F32)
    d_log = exact(from_here, at_ref[...] - lost, NN) + exact(from_here, at_t_ref[...], NT)
    d_log = d_log + jnp.sum(lost, axis=0, keepdims=True) + jnp.exp(cum[-1:]) * tail
    d_step_ref[...] = (direct - d_log * rate_ref[...]).T


def call(kernel, outs, *args, scalars=0, name="kernel"):
    vmem, smem = pl.BlockSpec(memory_space=pltpu.VMEM), pl.BlockSpec(memory_space=pltpu.SMEM)
    return pl.pallas_call(
        kernel,
        out_shape=[jax.ShapeDtypeStruct(shape, kind) for shape, kind in outs],
        in_specs=[smem] * scalars + [vmem] * (len(args) - scalars),
        out_specs=[vmem] * len(outs),
        compiler_params=pltpu.CompilerParams(vmem_limit_bytes=(24 if name == "normback" else 12) << 20),
    )(*args)


def swapped(x, axis, mask):
    n = lax.axis_size(axis)
    return lax.ppermute(x, axis, [(i, i ^ mask) for i in range(n)])


def bits_of(n):
    return [1 << k for k in range(n.bit_length() - 1)]


def reorder(blocks, me, n):
    blocks = list(blocks)
    for bit in bits_of(n):
        is_set = (me & bit) != 0
        for m in range(n):
            if not m & bit:
                a, b = blocks[m], blocks[m | bit]
                blocks[m], blocks[m | bit] = jnp.where(is_set, b, a), jnp.where(is_set, a, b)
    return blocks


def gather_relative(x, axis):
    n = lax.axis_size(axis)
    blocks = {0: x}
    for bit in reversed(bits_of(n)):
        for m in sorted(blocks):
            blocks[m | bit] = swapped(blocks[m], axis, bit)
    return [blocks[m] for m in range(n)]


def exchange_relative(blocks, axis):
    swaps = [swapped(blocks[m], axis, m) for m in range(1, len(blocks))]
    return [blocks[0]] + swaps


def gather_columns(x, axis):
    n = lax.axis_size(axis)
    return jnp.concatenate(reorder(gather_relative(x, axis), lax.axis_index(axis), n), axis=1)


def partner_kernel(width, spots, at_ref, x_ref, *refs):
    got_refs, out_ref = refs[:-1], refs[-1]
    for k in range(out_ref.shape[1] // width):
        start = pl.multiple_of(at_ref[0, k] * width, width)
        total = x_ref[:, pl.ds(start, width)].astype(F32)
        for got_ref, spot in zip(got_refs, spots):
            total = total + got_ref[:, spot[k] * width : (spot[k] + 1) * width].astype(F32)
        out_ref[:, k * width : (k + 1) * width] = total.astype(BF16)


def scatter_sum_columns(x, axis):
    n, me = lax.axis_size(axis), lax.axis_index(axis)
    width = x.shape[1] // n
    held, received = list(range(n)), []
    for bit in bits_of(n) + [0]:
        going = [m for m in held if m & bit] if bit else held
        spots = [[order.index(m) for m in going] for _, order in received]
        (sent,) = call(
            functools.partial(partner_kernel, width, spots),
            [((x.shape[0], width * len(going)), BF16)],
            jnp.stack([me ^ m for m in going]).astype(jnp.int32).reshape(1, -1),
            x,
            *[got for got, _ in received],
            scalars=1,
            name="sum",
        )
        if not bit:
            return sent
        held = [m for m in held if not m & bit]
        received.append((swapped(sent, axis, bit), held))


def exchange_steps(held, sent, axis, events):
    parts, sources = [held], [0]
    for bit in reversed(bits_of(held.shape[0])):
        if len(parts) > 1:
            rows = [part.reshape(-1, *part.shape[-3:])[:, bit : 2 * bit] for part in parts]
            sent = jnp.concatenate(rows, axis=0)
        got = swapped(sent, axis, bit)
        parts.append(after(got, events[len(parts) - 1]) if len(parts) <= len(events) else got)
        sources += [source | bit for source in sources]
    return parts, sources


def gather_steps(x, axis, moved):
    n = lax.axis_size(axis)
    offsets, blocks = [0], [x]
    for bit in reversed(bits_of(n)):
        for m, block in list(zip(offsets, blocks)):
            hop = bit
            if m in moved:
                hop = moved[m]
                block = blocks[offsets.index(m ^ hop ^ bit)]
            blocks.append(swapped(block, axis, hop))
            offsets.append(m | bit)
    return offsets, blocks


def after(x, *events):
    return lax.optimization_barrier((x, *events))[0]


def spread_states(own, widths, entering, forward, axis, name, seen=None):
    width, heads = widths
    n, me = lax.axis_size(axis), lax.axis_index(axis)
    bits = bits_of(n)
    state = []
    for step, bit in enumerate(bits):
        first, last = step == 0, bit == bits[-1]
        uses = ((me & bit) != 0) == forward
        use = jnp.where(uses, 1.0, 0.0).astype(F32).reshape(1, 1)
        args = [use, own, swapped(own, axis, bit)] + state
        outs = [((width, STATE), F32)]
        if last and forward:
            args.append(entering)
        if not last:
            outs = [(own.shape, BF16)] + outs + [((heads, LANES), F32)]
        made = call(functools.partial(join_kernel, first, last, forward), outs, *args, scalars=1, name=name + ("last" if last else "join"))
        if last:
            return made[0]
        own, state = made[0], list(made[1:])
        if seen is not None:
            seen.append(own)


def return_kernel(grad_ref, select_ref, *refs):
    blocks, out_ref = refs[:-1], refs[-1]
    total = grad_ref[...].astype(F32)
    for m, block in enumerate(blocks):
        total = total + mm(select_ref[m], block[...], TN)
    out_ref[...] = total.astype(BF16)


def proj_kernel(places, *refs):
    refs, out_ref = refs[:-1], refs[-1]
    normed, mixes = refs[: len(places)], refs[len(places) :]
    chunk = 2 * LANES
    rows = [mixes[0][0]]
    for mix in mixes[1:]:
        shape = mix.shape
        sources = shape[0] if len(shape) == 4 else 1
        rows += [mix[k, 0] if len(shape) == 4 else mix[0] for k in range(sources)]
    for c in range(0, out_ref.shape[0], chunk):
        total = jnp.zeros((chunk, out_ref.shape[1]), F32)
        for place, row in zip(places, rows):
            total = total + mm(normed[place][:, c : c + chunk], row, TN)
        out_ref[c : c + chunk, :] = total


def mix_kernel(place_ref, *refs):
    blocks, (mix_ref, sent_ref) = refs[:-2], refs[-2:]
    count, _, width = mix_ref.shape
    each = count // len(blocks)
    for m, block in enumerate(blocks):
        for part in range(each):
            at = place_ref[0, m * each + part]
            mix_ref[at] = block[:, part * width : (part + 1) * width]

            @pl.when(at >= count // 2)
            def _():
                sent_ref[at - count // 2] = block[:, part * width : (part + 1) * width]


def pack_kernel(experts, routes_ref, weight_ref, x_ref, grad_ref, packed_ref, select_ref):
    slots, tokens = select_ref.shape
    capacity = slots // experts
    width = x_ref.shape[1]
    numbers = iota((experts, tokens), 0)
    mask = jnp.zeros((experts, tokens), F32)
    weight = jnp.zeros((experts, tokens), F32)
    for k in range(routes_ref.shape[0]):
        chosen = routes_ref[k : k + 1, :] == numbers
        mask = jnp.where(chosen, 1.0, mask)
        weight = jnp.where(chosen, weight_ref[k : k + 1, :], weight)
    earlier = (iota((tokens, tokens), 0) < iota((tokens, tokens), 1)).astype(BF16)
    place = jnp.where(mask > 0.5, mm(mask.astype(BF16), earlier, NN), -1.0)
    row, number = iota((slots, experts), 0), iota((slots, experts), 1) * capacity
    owner = jnp.logical_and(row >= number, row < number + capacity).astype(F32)
    first = jnp.sum(owner * number.astype(F32), axis=1, keepdims=True)
    at_row = mm(owner.astype(BF16), place.astype(BF16), NN)
    at_slot = at_row + first == iota((slots, tokens), 0).astype(F32)
    at_slot = jnp.logical_and(at_slot, at_row > -0.5)
    of_row = exact(owner, weight, NN)
    slot_weight = jnp.sum(jnp.where(at_slot, of_row, 0.0), axis=1, keepdims=True)
    select = at_slot.astype(BF16)
    select_ref[...] = select
    packed_ref[:, :width] = mm(select, x_ref[...], NN).astype(BF16)
    packed_ref[:, width:] = (mm(select, grad_ref[...], NN) * slot_weight).astype(BF16)


def expert_hidden(routed_rows, routed_grads, w_gate, w_up, w_down):
    pre_gate = jnp.dot(routed_rows, w_gate, preferred_element_type=jnp.float32)
    pre_up = jnp.dot(routed_rows, w_up, preferred_element_type=jnp.float32)
    activated = jax.nn.silu(pre_gate)
    hidden = (activated * pre_up).astype(jnp.bfloat16)
    hidden_grad = lax.dot_general(
        routed_grads, w_down, (((1,), (1,)), ((), ())), preferred_element_type=jnp.float32
    )
    sigmoid_gate = jax.nn.sigmoid(pre_gate)
    gate_grad = (
        hidden_grad * pre_up * sigmoid_gate * (1.0 + pre_gate * (1.0 - sigmoid_gate))
    ).astype(jnp.bfloat16)
    up_grad = (hidden_grad * activated).astype(jnp.bfloat16)
    return (hidden, gate_grad, up_grad)


def expert_weight_grads(routed_rows, routed_grads, hidden, gate_grad, up_grad):
    contract = (((0,), (0,)), ((), ()))
    grad_g = lax.dot_general(routed_rows, gate_grad, contract, preferred_element_type=jnp.float32)
    grad_u = lax.dot_general(routed_rows, up_grad, contract, preferred_element_type=jnp.float32)
    grad_d = lax.dot_general(hidden, routed_grads, contract, preferred_element_type=jnp.float32)
    return (grad_g.astype(jnp.bfloat16), grad_u.astype(jnp.bfloat16), grad_d.astype(jnp.bfloat16))


def row_partial(gate_grad, up_grad, w_gate, w_up):
    contract = (((1,), (1,)), ((), ()))
    partial_sum = lax.dot_general(gate_grad, w_gate, contract, preferred_element_type=jnp.float32)
    partial_sum = partial_sum + lax.dot_general(
        up_grad, w_up, contract, preferred_element_type=jnp.float32
    )
    return partial_sum.astype(jnp.bfloat16)


def body(
    mixer_output_stream,
    layer_output_gradient,
    routes,
    expert_combine_weight,
    expert_gate_weight,
    expert_up_weight,
    expert_down_weight,
    head_mixer_input,
    head_step_size,
    head_decay_rate,
    extra_log_decay,
    state_entering_span,
    state_input_vectors,
    state_readout_vectors,
    gate_preactivation,
    group_norm_scale,
    mixer_output_weight,
):
    expert_count, me = lax.axis_size("sp"), lax.axis_index("sp")
    local_tokens, heads = head_step_size.shape
    width = head_mixer_input.shape[1]
    vectors = state_input_vectors.shape[1]
    capacity = 3 * local_tokens // expert_count
    w_gate = expert_gate_weight[0]
    w_up = expert_up_weight[0]
    w_down = expert_down_weight[0]
    rate = head_decay_rate[None, :]
    gain = group_norm_scale[None, :]
    entering = state_entering_span.reshape(width, STATE)

    slots = expert_count * capacity
    packed, select = call(
        functools.partial(pack_kernel, expert_count),
        [((slots, 2 * mixer_output_stream.shape[1]), BF16), ((slots, local_tokens), BF16)],
        routes.T ^ me,
        expert_combine_weight.T,
        mixer_output_stream,
        layer_output_gradient,
        name="pack",
    )
    packed, step_size = lax.optimization_barrier((packed, head_step_size))
    scan_args = (head_mixer_input, step_size, rate, extra_log_decay)
    rows = packed.reshape(expert_count, capacity, -1)
    received = exchange_relative([rows[m] for m in range(expert_count)], "sp")

    (own_state,) = call(
        state_kernel, [((width + heads, STATE), BF16)], *scan_args, state_input_vectors
    )
    part_width = mixer_output_stream.shape[1]
    got_rows = jnp.concatenate([part[:, :part_width] for part in received], axis=0)
    got_grads = jnp.concatenate([part[:, part_width:] for part in received], axis=0)
    routed_rows = gather_columns(got_rows, "tp")
    routed_grads = gather_columns(got_grads, "tp")
    hidden, gate_grad, up_grad = expert_hidden(routed_rows, routed_grads, w_gate, w_up, w_down)
    partial_rows = row_partial(gate_grad, up_grad, w_gate, w_up)
    summed = scatter_sum_columns(partial_rows, "tp")
    offsets, weights = gather_steps(after(mixer_output_weight, got_rows), "sp", {})
    incoming = spread_states(
        own_state, (width, heads), entering, True, "sp", "f"
    )
    scan_out, normed = call(
        scan_kernel,
        [((local_tokens, width), F32), ((local_tokens, width), BF16)],
        *scan_args,
        state_input_vectors,
        state_readout_vectors,
        after(incoming, summed),
        gate_preactivation,
        gain,
    )
    summed = summed.reshape(expert_count, capacity, -1)
    returned = exchange_relative([summed[m] for m in range(expert_count)], "sp")
    (own_cols,) = call(
        return_kernel,
        [(layer_output_gradient.shape, BF16)],
        layer_output_gradient,
        select.reshape(expert_count, capacity, local_tokens),
        *returned,
        name="back",
    )
    grad_g, grad_u, grad_d = expert_weight_grads(
        routed_rows, routed_grads, hidden, gate_grad, up_grad
    )
    own_parts = gather_relative(own_cols, "tp")
    out_width = mixer_output_weight.shape[1]
    each = part_width // out_width
    numbers = jnp.arange(expert_count, dtype=jnp.int32)
    place = me ^ (((numbers // each) ^ lax.axis_index("tp")) * each + numbers % each)
    mix_parts, mix_sent = call(
        mix_kernel,
        [
            ((expert_count, local_tokens, out_width), BF16),
            ((expert_count // 2, local_tokens, out_width), BF16),
        ],
        place.reshape(1, -1),
        *own_parts,
        scalars=1,
        name="mix",
    )

    scan_grad, gate_grad_in, reached = call(
        functools.partial(norm_back_kernel, expert_count),
        [((local_tokens, width), BF16)] * 2 + [((width + heads, STATE), BF16)],
        *scan_args[1:],
        state_readout_vectors,
        scan_out,
        gate_preactivation,
        gain,
        mix_parts,
        *[weights[offsets.index(m)] for m in range(expert_count)],
        name="normback",
    )
    joined = []
    later = spread_states(reached, (width, heads), None, False, "sp", "b", joined)
    inner_x_grad, c_grad, inner_b_grad, at, at_t = call(
        inner_back_kernel,
        [
            ((local_tokens, width), F32),
            ((local_tokens, vectors), BF16),
            ((local_tokens, vectors), F32),
            ((local_tokens, heads), F32),
            ((heads, local_tokens), F32),
        ],
        *scan_args,
        state_input_vectors,
        state_readout_vectors,
        incoming,
        scan_grad,
        name="inner",
    )
    kept, all_normed = gather_steps(normed, "sp", {6: 2})
    all_mix, sources = exchange_steps(mix_parts, mix_sent, "sp", (grad_d, grad_u))
    input_grad, step_grad, b_grad = call(
        last_back_kernel,
        [
            ((local_tokens, width), BF16),
            ((heads, local_tokens), F32),
            ((local_tokens, vectors), BF16),
        ],
        *scan_args,
        state_input_vectors,
        incoming,
        later,
        inner_x_grad,
        inner_b_grad,
        at,
        at_t,
    )
    all_normed[-1] = after(all_normed[-1], step_grad)
    (proj_grad,) = call(
        functools.partial(proj_kernel, [kept.index(m) for m in sources]),
        [((width, out_width), F32)],
        *all_normed,
        *all_mix,
        name="proj",
    )
    return (
        grad_g[None],
        grad_u[None],
        grad_d[None],
        proj_grad,
        input_grad,
        step_grad.T,
        b_grad,
        c_grad,
        gate_grad_in,
    )


def solution(mesh):
    return jax.shard_map(
        body,
        mesh=mesh,
        in_specs=(
            P("sp", "tp"),
            P("sp", "tp"),
            P("sp", None),
            P("sp", None),
            P("sp", None, "tp"),
            P("sp", None, "tp"),
            P("sp", "tp", None),
            P("sp", "tp"),
            P("sp", "tp"),
            P("tp"),
            P("sp", "tp"),
            P("tp", None, None),
            P("sp", "tp"),
            P("sp", "tp"),
            P("sp", "tp"),
            P("tp"),
            P("tp", "sp"),
        ),
        out_specs=(
            P("sp", None, "tp"),
            P("sp", None, "tp"),
            P("sp", "tp", None),
            P("tp", "sp"),
            P("sp", "tp"),
            P("sp", "tp"),
            P("sp", "tp"),
            P("sp", "tp"),
            P("sp", "tp"),
        ),
        check_vma=False,
    )
```
